32 devices in a mesh: fs: 16 (over z, y, x), tp: 2 (over core).
Axes of the slice: x: 2, y: 2, z: 4, core: 2. Of those that a mesh axis runs over, the one named last changes fastest.
Arguments:
- x_late: bfloat16 [3072, 2048], P(('fs', 'tp')), may hold values from -6 to 6
- x_early: bfloat16 [3072, 2048], P(('fs', 'tp')), may hold values from -6 to 6
- cotangent: bfloat16 [3072, 2048], P(('fs', 'tp')), may hold values from -0.3984375 to 0.3984375
- norm_gain: bfloat16 [2048], replicated, may hold values from 0.099609375 to 1.8984375
- gate_weight: bfloat16 [2048, 2816], P('fs', 'tp'), may hold values from -0.125 to 0.125
- up_weight: bfloat16 [2048, 2816], P('fs', 'tp'), may hold values from -0.125 to 0.125
- down_weight: bfloat16 [2048, 2816], P('fs', 'tp'), may hold values from -0.109375 to 0.109375
- gate_sum: float32 [2048, 2816], P('fs', 'tp'), may hold values from -6 to 6
- up_sum: float32 [2048, 2816], P('fs', 'tp'), may hold values from -6 to 6
- down_sum: float32 [2048, 2816], P('fs', 'tp'), may hold values from -6 to 6
Outputs:
- out_late: bfloat16 [3072, 2048], P(('fs', 'tp'))
- grad_early: bfloat16 [3072, 2048], P(('fs', 'tp'))
- gate_sum_out: float32 [2048, 2816], P('fs', 'tp')
- up_sum_out: float32 [2048, 2816], P('fs', 'tp')
- down_sum_out: float32 [2048, 2816], P('fs', 'tp')
The draws below stay inside these ranges and needn't reach their ends.
All inputs are finite; a program needn't handle non-finite values.
Results may differ from the reference program's by a relative error of at most 0.0095.
Values may be sent and summed in bfloat16 or wider, within the bound.
A program may use at most 128 MiB of HBM per device.

```python
import jax
import jax.numpy as jnp
from jax import lax

D = 2048
FF = 2816
TOKENS = 3072
N_TP = 2


def strengthened(array, key, source, target, shards_of, factor):
    owner, partner = [(jnp.arange(array.shape[dim]) // (array.shape[dim] // shards_of)).reshape([-1 if axis == dim else 1 for axis in range(array.ndim)]) for dim in (source, target)]
    chosen = jax.random.permutation(key, shards_of)[partner]
    strong = (owner == chosen) | (owner == (partner + shards_of // 2) % shards_of)
    return jnp.where(strong, factor * array, array)


def block_levels(key, dims, pieces, low, top_value):
    def one(axis_at, parts):
        heights = jax.random.uniform(jax.random.fold_in(jax.random.fold_in(key, 6), axis_at), (parts,), jnp.float32, low / len(pieces), top_value / len(pieces))
        return jnp.repeat(jnp.exp(heights), dims[axis_at] // parts).reshape((-1,) + (1,) * (len(dims) - axis_at - 1))

    loudness = one(*pieces[0])
    for cut in pieces[1:]:
        loudness = loudness * one(*cut)
    return loudness


def normal_values(rng, shape, deviation, reach, split=(), dtype=jnp.bfloat16):
    drawn = deviation * jax.random.normal(rng, shape, jnp.float32)
    if split:
        drawn = drawn * block_levels(rng, shape, split, -0.22, 0.18)
    return jnp.clip(drawn, -reach, reach).astype(dtype)


def noise_with(key, dims, scale, limit, pieces, heavy, kind=jnp.bfloat16):
    entries = scale * jax.random.normal(key, dims, jnp.float32)
    if pieces:
        entries = entries * block_levels(key, dims, pieces, -0.22, 0.18)
    return jnp.clip(strengthened(entries, jax.random.fold_in(key, 3), *heavy), -limit, limit).astype(kind)


def setup_inputs(seed: int = 0) -> dict:
    key_of = jax.random.split(jax.random.key(seed), 11)
    x_late = normal_values(key_of[0], (TOKENS, D), 1.0, 6.0, ((0, 32),))
    x_early = normal_values(key_of[1], (TOKENS, D), 1.0, 6.0, ((0, 32),))
    cotangent = noise_with(key_of[2], (TOKENS, D), 0.05, 0.3984375, ((0, 32),), (0, 1, 32, 2.75))
    norm_gain = jnp.clip(1.0 + 0.18 * jax.random.normal(key_of[3], (D,), jnp.float32), 0.099609375, 1.8984375).astype(jnp.bfloat16)
    gate_weight = normal_values(key_of[4], (D, FF), D ** -0.5, 0.125, ((0, 16), (1, 2)))
    up_weight = normal_values(key_of[5], (D, FF), D ** -0.5, 0.125, ((0, 16), (1, 2)))
    down_weight = normal_values(key_of[6], (D, FF), FF ** -0.5, 0.109375, ((0, 16), (1, 2)))
    gate_sum = normal_values(key_of[7], (D, FF), 1.0, 6.0, ((0, 16), (1, 2)), jnp.float32)
    up_sum = normal_values(key_of[8], (D, FF), 1.0, 6.0, ((0, 16), (1, 2)), jnp.float32)
    down_sum = normal_values(key_of[9], (D, FF), 1.0, 6.0, ((0, 16), (1, 2)), jnp.float32)
    return {"x_late": x_late, "x_early": x_early, "cotangent": cotangent, "norm_gain": norm_gain, "gate_weight": gate_weight, "up_weight": up_weight, "down_weight": down_weight, "gate_sum": gate_sum, "up_sum": up_sum, "down_sum": down_sum}


eps = 1e-06

def normalize(x, norm_gain):
    xf = x.astype(jnp.float32)
    inv = lax.rsqrt(lax.optimization_barrier(jnp.mean(xf * xf, axis=-1, keepdims=True)) + eps)
    return (xf, inv, (xf * inv * norm_gain.astype(jnp.float32)).astype(jnp.bfloat16))

def block_sum(pairs):
    width = FF // N_TP
    total = jnp.zeros((pairs[0][0].shape[0], pairs[0][1].shape[0]), jnp.float32)
    for block in range(N_TP):
        part = jnp.zeros_like(total)
        for left, right in pairs:
            part = part + jnp.dot(left[:, block * width:(block + 1) * width], right[:, block * width:(block + 1) * width].T, preferred_element_type=jnp.float32)
        rounded = lax.optimization_barrier(part.astype(jnp.bfloat16))
        total = total + rounded.astype(jnp.float32)
    return total

def reference(x_late, x_early, cotangent, norm_gain, gate_weight, up_weight, down_weight, gate_sum, up_sum, down_sum):
    late_f, late_inv, normed_late = normalize(x_late, norm_gain)
    gate_l = jnp.dot(normed_late, gate_weight, preferred_element_type=jnp.float32)
    up_l = jnp.dot(normed_late, up_weight, preferred_element_type=jnp.float32)
    hidden_l = (jax.nn.silu(gate_l) * up_l).astype(jnp.bfloat16)
    branch = block_sum([(hidden_l, down_weight)])
    out_late = (late_f + 0.5 * branch).astype(jnp.bfloat16)
    early_f, inv, normed_early = normalize(x_early, norm_gain)
    gate_e = jnp.dot(normed_early, gate_weight, preferred_element_type=jnp.float32)
    up_e = jnp.dot(normed_early, up_weight, preferred_element_type=jnp.float32)
    sig = jax.nn.sigmoid(gate_e)
    silu_e = gate_e * sig
    hidden_e = (silu_e * up_e).astype(jnp.bfloat16)
    half_cot = (0.5 * cotangent.astype(jnp.float32)).astype(jnp.bfloat16)
    down_grad = jnp.dot(half_cot.T, hidden_e, preferred_element_type=jnp.float32)
    d_hidden = jnp.dot(half_cot, down_weight, preferred_element_type=jnp.float32)
    d_gate = (d_hidden * up_e * sig * (1.0 + gate_e * (1.0 - sig))).astype(jnp.bfloat16)
    d_up = (d_hidden * silu_e).astype(jnp.bfloat16)
    gate_grad = jnp.dot(normed_early.T, d_gate, preferred_element_type=jnp.float32)
    up_grad = jnp.dot(normed_early.T, d_up, preferred_element_type=jnp.float32)
    d_normed = block_sum([(d_gate, gate_weight), (d_up, up_weight)])
    scaled = d_normed * norm_gain.astype(jnp.float32)
    d_input = inv * scaled - early_f * inv ** 3 * lax.optimization_barrier(jnp.mean(scaled * early_f, axis=-1, keepdims=True))
    grad_early = (cotangent.astype(jnp.float32) + d_input).astype(jnp.bfloat16)
    return (out_late, grad_early, gate_sum + gate_grad, up_sum + up_grad, down_sum + down_grad)
```

```python
import jax
import jax.numpy as jnp
from jax import lax
from jax.sharding import Mesh
from jax.sharding import PartitionSpec as P

eps = 1e-06


def normalize(x, gain):
    xf = x.astype(jnp.float32)
    inv = lax.rsqrt(jnp.mean(xf * xf, axis=-1, keepdims=True) + eps)
    return (inv, (xf * inv * gain).astype(jnp.bfloat16))


def contract_last(left, right):
    return lax.dot_general(
        left, right, (((1,), (1,)), ((), ())), preferred_element_type=jnp.float32
    )


def contract_first(left, right):
    return lax.dot_general(
        left, right, (((0,), (0,)), ((), ())), preferred_element_type=jnp.float32
    )


def dot(left, right):
    return jnp.dot(left, right, preferred_element_type=jnp.float32)


def make_on_device(split, n_tp):
    def shifted(value, axis, size, step):
        return lax.ppermute(value, axis, [(i, (i + step) % size) for i in range(size)])

    def gather_tokens(own):
        over_fi = [own] + [shifted(own, "fi", split, k) for k in range(1, split)]
        chip = jnp.concatenate(over_fi, axis=1)
        over_tp = [chip] + [shifted(chip, "tp", n_tp, j) for j in range(1, n_tp)]
        return jnp.concatenate(over_tp, axis=1)

    def scatter_tokens(part):
        blocks = part.astype(jnp.bfloat16).reshape((n_tp, split, -1, part.shape[-1]))
        mine = blocks[0].astype(jnp.float32)
        for j in range(1, n_tp):
            mine = mine + shifted(blocks[j], "tp", n_tp, -j).astype(jnp.float32)
        total = mine[0]
        if split > 1:
            sent = mine[1:].astype(jnp.bfloat16)
            for k in range(1, split):
                total = total + shifted(sent[k - 1], "fi", split, -k).astype(jnp.float32)
        return total

    def gather_weight(parts):
        rows, cols = parts[0].shape
        width = cols // split
        if split > 1:
            pieces = [p.reshape(rows, split, width).transpose(1, 0, 2) for p in parts]
            sent = jnp.concatenate(pieces, axis=2) if len(pieces) > 1 else pieces[0]
            sent = lax.all_to_all(sent, "fi", split_axis=0, concat_axis=0, tiled=True)
            sent = sent.reshape(split * rows, len(parts) * width)
        else:
            sent = jnp.concatenate(parts, axis=1) if len(parts) > 1 else parts[0]
        return lax.all_gather(sent, "fo", axis=0, tiled=True)

    def scatter_grad(grad, sums):
        rows, cols = sums[0].shape
        width = cols // split
        part = lax.psum_scatter(
            grad.astype(jnp.bfloat16), "fo", scatter_dimension=0, tiled=True
        )
        part = part.reshape(split, rows, len(sums) * width)
        if split > 1:
            part = lax.all_to_all(part, "fi", split_axis=0, concat_axis=0, tiled=True)
        outs = []
        for i, s in enumerate(sums):
            own = part[:, :, i * width : (i + 1) * width]
            own = own.transpose(1, 0, 2).reshape(rows, cols)
            outs.append(s + own.astype(jnp.float32))
        return outs

    def on_device(
        x_late,
        x_early,
        cotangent,
        norm_gain,
        gate_weight,
        up_weight,
        down_weight,
        gate_sum,
        up_sum,
        down_sum,
    ):
        width = gate_weight.shape[1] // split
        gain = norm_gain.astype(jnp.float32)
        inv_own, early_own = normalize(x_early, gain)
        _, late_own = normalize(x_late, gain)
        cot_own = (0.5 * cotangent.astype(jnp.float32)).astype(jnp.bfloat16)
        w_gu = gather_weight([gate_weight, up_weight])
        early_side = gather_tokens(jnp.stack([early_own, cot_own]))
        normed_early, half_cot = early_side[0], early_side[1]
        normed_late = gather_tokens(late_own[None])[0]
        w_down = gather_weight([down_weight])

        gu_e = dot(normed_early, w_gu)
        gate_e, up_e = gu_e[:, :width], gu_e[:, width:]
        sig = jax.nn.sigmoid(gate_e)
        silu_e = gate_e * sig
        hidden_e = (silu_e * up_e).astype(jnp.bfloat16)
        down_part = contract_first(half_cot, hidden_e)
        gu_l = dot(normed_late, w_gu)
        hidden_l = (jax.nn.silu(gu_l[:, :width]) * gu_l[:, width:]).astype(jnp.bfloat16)

        d_hidden = dot(half_cot, w_down)
        d_gate = (d_hidden * up_e * sig * (1.0 + gate_e * (1.0 - sig))).astype(jnp.bfloat16)
        d_up = (d_hidden * silu_e).astype(jnp.bfloat16)
        d_gu = jnp.concatenate([d_gate, d_up], axis=1)
        gu_part = contract_first(normed_early, d_gu)

        (down_out,) = scatter_grad(down_part, [down_sum])
        gate_out, up_out = scatter_grad(gu_part, [gate_sum, up_sum])

        d_normed = scatter_tokens(contract_last(d_gu, w_gu))
        branch = scatter_tokens(contract_last(hidden_l, w_down))
        out_late = (x_late.astype(jnp.float32) + 0.5 * branch).astype(jnp.bfloat16)
        early_f = x_early.astype(jnp.float32)
        scaled = d_normed * gain
        d_input = inv_own * scaled - early_f * inv_own**3 * jnp.mean(
            scaled * early_f, axis=-1, keepdims=True
        )
        grad_early = (cotangent.astype(jnp.float32) + d_input).astype(jnp.bfloat16)
        return (out_late, grad_early, gate_out, up_out, down_out)

    return on_device


WANTED = 8


def solution(mesh):
    n_fs, n_tp = mesh.shape["fs"], mesh.shape["tp"]
    split = max(1, WANTED // n_tp)
    while n_fs % split:
        split //= 2
    fine = Mesh(mesh.devices.reshape(n_fs // split, split, n_tp), ("fo", "fi", "tp"))
    tokens, rows = P(("fo", "fi", "tp"), None), P(("fo", "fi"), "tp")
    return jax.shard_map(
        make_on_device(split, n_tp),
        mesh=fine,
        in_specs=(tokens, tokens, tokens, P()) + (rows,) * 6,
        out_specs=(tokens, tokens, rows, rows, rows),
        check_vma=False,
    )
```
